32 devices in a mesh: grp: 2 (over y), fs: 8 (over z, core), tp: 2 (over x).
Axes of the slice: x: 2, y: 2, z: 4, core: 2. Of those that a mesh axis runs over, the one named last changes fastest.
Arguments:
- tokens: bfloat16 [3584, 2048], P(('grp', 'fs'), 'tp'), parts along dimension 0, may hold values from -170 to 170
- routes: int32 [3584, 6], P(('grp', 'fs')), parts along dimension 0, may hold values from 0 to 15, all different within a row; in each aligned block of 224 rows (0 to 223, 224 to 447, ...) at most 112 rows name the same one
- route_weights: float32 [3584, 6], P(('grp', 'fs')), parts along dimension 0, may hold values from 0.2 to 1
- norm_gain: float32 [2048], P('fs'), may hold values from 0.1 to 1.9
- gate_experts: float32 [16, 2048, 512], P(None, 'fs', 'tp'), may hold values from -0.125 to 0.125
- up_experts: float32 [16, 2048, 512], P(None, 'fs', 'tp'), may hold values from -0.125 to 0.125
- down_experts: float32 [16, 512, 2048], P(None, 'fs', 'tp'), may hold values from -0.25 to 0.25
- shared_gate: float32 [2048, 512], P('fs', 'tp'), may hold values from -0.125 to 0.125
- shared_up: float32 [2048, 512], P('fs', 'tp'), may hold values from -0.125 to 0.125
- shared_down: float32 [512, 2048], P('fs', 'tp'), may hold values from -0.25 to 0.25
Outputs:
- mixed: bfloat16 [3584, 2048], P(('grp', 'fs'), 'tp'), parts along dimension 0
- gate_ready: bfloat16 [32, 2048, 512], P(('grp', 'fs'), None, 'tp'), parts along dimension 0
- up_ready: bfloat16 [32, 2048, 512], P(('grp', 'fs'), None, 'tp'), parts along dimension 0
- down_ready: bfloat16 [32, 512, 2048], P(('grp', 'fs'), 'tp'), parts along dimension 0
- shared_gate_ready: bfloat16 [4096, 512], P('grp', 'tp'), parts along dimension 0
- shared_up_ready: bfloat16 [4096, 512], P('grp', 'tp'), parts along dimension 0
- shared_down_ready: bfloat16 [1024, 2048], P(('grp', 'tp')), parts along dimension 0
The draws below stay inside these ranges and needn't reach their ends.
There are 2 independent parts, one for each index of `grp`. The reference program is written for one: setup_inputs(seed, part) draws one part's arguments, and reference() takes and returns one part's arrays. A program takes and returns all parts, laid end to end along the dimension named above; an argument that names none is the same for every part. Nothing has to cross between parts.
Inputs may be any that keep to these rules, and one draw needn't show every extreme that they name: `routes`: the 6 experts of a row differ; among the rows of one index of fs no expert is named more than 112 times, a bound that some block reaches.
All inputs are finite; a program needn't handle non-finite values.
Results may differ from the reference program's by a relative error of at most 0.013.
Values may be sent and summed in bfloat16 or wider, within the bound.
A program may use at most 128 MiB of HBM per device.

```python
import math
import jax
import jax.numpy as jnp
import numpy as np
from jax import lax

D = 2048
FF = 512
SF = 512
EXPERTS = 16
TOP_K = 6
TOK_DEV = 224
TOKENS = 1792
CAP = 112
N_TP = 2


def draw_tokens(key, part):
    key_rows = jax.random.fold_in(key, 11)
    key_cols = jax.random.fold_in(key, 12)
    key_base = jax.random.fold_in(key, 13)
    row_scale = jnp.exp(jax.random.uniform(key_rows, (TOKENS, 1), jnp.float32, 0.0, math.log(10.0)))
    col_scale = jnp.exp(jax.random.uniform(key_cols, (1, D), jnp.float32, 0.0, math.log(10.0)))
    base = jnp.clip(jax.random.normal(key_base, (TOKENS, D), jnp.float32), -5.0, 5.0)
    return (base * row_scale * col_scale / 3.0).astype(jnp.bfloat16)


def block_scale(own_key, dims, cuts, low, top_value):
    def one(dim, blocks):
        steps = jax.random.uniform(jax.random.fold_in(jax.random.fold_in(own_key, 6), dim), (blocks,), jnp.float32, low / len(cuts), top_value / len(cuts))
        return jnp.repeat(jnp.exp(steps), dims[dim] // blocks).reshape((-1,) + (1,) * (len(dims) - dim - 1))

    gain = one(*cuts[0])
    for cut in cuts[1:]:
        gain = gain * one(*cut)
    return gain


def shared_out(rng, own, number, rows, amount, top, most, slope):
    order = jax.random.permutation(rng, amount)
    heavy_load, common = portions_of(amount, rows * top, most, slope, True), portions_of(amount, rows * top, most, slope, False)
    places = jnp.arange(amount)

    def named(lengths, turn):
        used = int((lengths > 0).sum())
        fixed = max(1, used // 4)
        passed = fixed + (places - fixed + turn * (used - fixed)) % max(1, amount - fixed)
        return jnp.zeros((amount,), jnp.int32).at[order[jnp.where(places < fixed, places, passed)]].set(jnp.asarray(lengths, jnp.int32))

    lengths = jnp.where(number % 4 == 0, named(heavy_load, number // 4), named(common, number - number // 4 - 1))
    mixed = jax.random.permutation(jax.random.fold_in(own, 3), amount)
    giver, receiver = mixed[0:amount // 2 * 2:2], mixed[1:amount // 2 * 2:2]
    room = jnp.minimum(lengths[giver] - 1, most - lengths[receiver]) // 2
    room = jnp.where((giver == order[0]) | (receiver == order[0]) | (lengths[receiver] == 0), 0, jnp.maximum(room, 0))
    passed = jax.random.randint(jax.random.fold_in(own, 4), (amount // 2,), 0, 1 << 20) % (room + 1)
    lengths = lengths.at[giver].add(-passed).at[receiver].add(passed)
    members = jnp.searchsorted(jnp.cumsum(lengths), jnp.arange(rows * top), side="right").astype(jnp.int32)
    grid = members.reshape(top, rows).T
    grid = grid[jax.random.permutation(jax.random.fold_in(own, 1), rows)]
    turn = jax.random.randint(jax.random.fold_in(own, 2), (rows, 1), 0, top)
    return jnp.take_along_axis(grid, (jnp.arange(top)[None, :] + turn) % top, axis=1)


def portions_of(amount, total, reach, skew, full):
    portions = [(1 << 20) // math.isqrt(rank ** skew) + 1 for rank in range(1, amount + 1)]
    largest = reach if full else min(reach, max(-(-total // amount), total * portions[0] // sum(portions)))
    least = 1 if total - largest >= amount - 1 else 0
    counts, spare = [largest] + [least] * (amount - 1), total - largest - least * (amount - 1)
    while spare > 0:
        movable = [i for i in range(1, amount) if counts[i] < largest] or [i for i in range(1, amount) if counts[i] < reach]
        pool, left = sum([portions[i] for i in movable]), spare
        for i in movable:
            addition = min(reach - counts[i], max(1, left * portions[i] // pool), spare)
            counts[i] = counts[i] + addition
            spare = spare - addition
    return np.array(counts)


def normal_values(stream_key, shape, scale, most, pieces=(), kind=jnp.bfloat16):
    factor_of = block_scale(stream_key, shape, pieces, -0.22, 0.18) if pieces else 1.0
    array = jax.random.normal(stream_key, shape, jnp.float32) * scale * factor_of
    return jnp.minimum(jnp.maximum(array, -most), most).astype(kind)


def setup_inputs(seed: int = 0, part: int = 0) -> dict:
    splits = jax.random.split(jax.random.key(seed), 11)
    part_splits = jax.random.split(jax.random.fold_in(splits[10], part), 11)
    tokens = draw_tokens(jax.random.fold_in(jax.random.fold_in(splits[10], part), 71), part)
    routes_keys = jax.random.split(jax.random.fold_in(part_splits[1], 1), TOKENS // TOK_DEV)
    routes_turns = jax.random.permutation(jax.random.fold_in(part_splits[1], 3), TOKENS // TOK_DEV)
    routes = jax.vmap(lambda own, number: shared_out(jax.random.fold_in(part_splits[1], 2), own, number, TOK_DEV, EXPERTS, TOP_K, CAP, 1))(routes_keys, routes_turns).reshape((TOKENS, TOP_K))
    route_weights = jnp.clip(jnp.exp(math.log(1.0) - 1.609438 * jax.random.uniform(part_splits[2], (TOKENS, TOP_K), jnp.float32) ** block_scale(part_splits[2], (TOKENS, TOP_K), ((0, 8),), -0.2, 0.2)), 0.2, 1.0)
    norm_gain = jnp.clip(1.0 + 0.18 * jax.random.normal(splits[3], (D,), jnp.float32), 0.1, 1.9)
    gate_experts = normal_values(splits[4], (EXPERTS, D, FF), D ** -0.5, 0.125, ((1, 8), (2, 2)), jnp.float32)
    up_experts = normal_values(splits[5], (EXPERTS, D, FF), D ** -0.5, 0.125, ((1, 8), (2, 2)), jnp.float32)
    down_experts = normal_values(splits[6], (EXPERTS, FF, D), FF ** -0.5, 0.25, ((1, 8), (2, 2)), jnp.float32)
    shared_gate = normal_values(splits[7], (D, SF), D ** -0.5, 0.125, ((0, 8), (1, 2)), jnp.float32)
    shared_up = normal_values(splits[8], (D, SF), D ** -0.5, 0.125, ((0, 8), (1, 2)), jnp.float32)
    shared_down = normal_values(splits[9], (SF, D), SF ** -0.5, 0.25, ((0, 8), (1, 2)), jnp.float32)
    return {"tokens": tokens, "routes": routes, "route_weights": route_weights, "norm_gain": norm_gain, "gate_experts": gate_experts, "up_experts": up_experts, "down_experts": down_experts, "shared_gate": shared_gate, "shared_up": shared_up, "shared_down": shared_down}


def grouped_product(active, weight):
    groups = N_TP
    span_cols = active.shape[1] // groups
    totals = jnp.zeros((active.shape[0], weight.shape[1]), jnp.float32)
    for section in range(groups):
        product = jnp.dot(active[:, section * span_cols:(section + 1) * span_cols], weight[section * span_cols:(section + 1) * span_cols], preferred_element_type=jnp.float32)
        rounded = lax.optimization_barrier(product.astype(jnp.bfloat16))
        totals = totals + rounded.astype(jnp.float32)
    return totals

def reference(tokens, routes, route_weights, norm_gain, gate_experts, up_experts, down_experts, shared_gate, shared_up, shared_down):
    gate_ready = (gate_experts * norm_gain[None, :, None]).astype(jnp.bfloat16)
    up_ready = (up_experts * norm_gain[None, :, None]).astype(jnp.bfloat16)
    down_ready = down_experts.astype(jnp.bfloat16)
    shared_gate_ready = (shared_gate * norm_gain[:, None]).astype(jnp.bfloat16)
    shared_up_ready = (shared_up * norm_gain[:, None]).astype(jnp.bfloat16)
    shared_down_ready = shared_down.astype(jnp.bfloat16)
    widened = tokens.astype(jnp.float32)
    normed = (widened * lax.rsqrt(lax.optimization_barrier(jnp.mean(widened * widened, axis=1, keepdims=True)) + 1e-06)).astype(jnp.bfloat16)
    shared_active = (jax.nn.silu(jnp.dot(normed, shared_gate_ready, preferred_element_type=jnp.float32)) * jnp.dot(normed, shared_up_ready, preferred_element_type=jnp.float32)).astype(jnp.bfloat16)
    shared_rows = grouped_product(shared_active, shared_down_ready)
    blocks = TOKENS // TOK_DEV
    pairs = TOK_DEV * TOP_K
    block_routes = routes.reshape(blocks, pairs)
    onehot = (block_routes[:, :, None] == jnp.arange(EXPERTS, dtype=jnp.int32)[None, None, :]).astype(jnp.int32)
    earlier = jnp.cumsum(onehot, axis=1) - onehot
    slot_index = lax.optimization_barrier(jnp.sum(earlier * onehot, axis=2)).astype(jnp.int32)
    target = block_routes * CAP + slot_index
    token_index = (jnp.arange(TOKENS * TOP_K, dtype=jnp.int32) // TOP_K).astype(jnp.int32)
    flat_target = (target + (jnp.arange(blocks, dtype=jnp.int32) * (EXPERTS * CAP))[:, None]).reshape(-1)
    source = jnp.full((blocks * EXPERTS * CAP,), -1, jnp.int32).at[flat_target].set(token_index)
    source = source.reshape(blocks, EXPERTS, CAP).transpose(1, 0, 2).reshape(EXPERTS, blocks * CAP)

    def expert_rows(operands):
        row_index, gate_one, up_one, down_one = operands
        present = row_index >= 0
        inputs = jnp.where(present[:, None], normed[jnp.maximum(row_index, 0)], jnp.zeros((), jnp.bfloat16))
        active = (jax.nn.silu(jnp.dot(inputs, gate_one, preferred_element_type=jnp.float32)) * jnp.dot(inputs, up_one, preferred_element_type=jnp.float32)).astype(jnp.bfloat16)
        return grouped_product(active, down_one).astype(jnp.bfloat16)
    results = lax.map(expert_rows, (source, gate_ready, up_ready, down_ready))
    flat_results = results.reshape(EXPERTS * blocks * CAP, D)
    block_of = (jnp.arange(TOKENS, dtype=jnp.int32) // TOK_DEV)[:, None]
    position = routes * (blocks * CAP) + block_of * CAP + slot_index.reshape(TOKENS, TOP_K)
    mixed = shared_rows
    for choice_k in range(TOP_K):
        mixed = mixed + flat_results[position[:, choice_k]].astype(jnp.float32) * route_weights[:, choice_k:choice_k + 1]
    return (mixed.astype(jnp.bfloat16), gate_ready, up_ready, down_ready, shared_gate_ready, shared_up_ready, shared_down_ready)
```

```python
import functools

import jax
import jax.numpy as jnp
from jax import lax
from jax.experimental import pallas as pl
from jax.experimental.pallas import tpu as pltpu
from jax.sharding import PartitionSpec as P

MESH = pl.DeviceIdType.MESH


def move_kernel(sizes, *refs):
    groups, n, tps = sizes
    chips, band = n // 2, n // tps
    half = band // 2
    tok_in, sc_in = refs[:2]
    srcs = refs[2:8]
    tok, sc = refs[8:10]
    outs = refs[10:16]
    (
        own_s, lz_s, lz_r, ls_s, ls_r, lx_s, lx_r, ly_s, ly_r,
        e_s, e_r, p_s, p_r, d_s, d_r, dy_s, dy_r, ds_s, ds_r,
    ) = refs[16:]
    grp, fs, tp = lax.axis_index("grp"), lax.axis_index("fs"), lax.axis_index("tp")
    z, c = fs // 2, lax.rem(fs, 2)
    home = fs // band
    cols = tok_in.shape[1]
    both = fs + 1 - 2 * c

    def at(g, f, t):
        return {"grp": g, "fs": f, "tp": t}

    def turn(v, by, size):
        return lax.rem(v + by + size, size)

    def remote(src, dst, ssem, rsem, where):
        return pltpu.make_async_remote_copy(
            src_ref=src, dst_ref=dst, send_sem=ssem, recv_sem=rsem, device_id=where, device_id_type=MESH
        )

    def arrived(block, rsem):
        remote(block, block, rsem, rsem, at(grp, both, tp)).wait_recv()

    def span(start, size):
        return pl.ds(pl.multiple_of(start * size, size), size)

    def tok_at(f, x):
        return tok.at[f, :, span(x, cols)]

    own = [
        pltpu.make_async_copy(tok_in, tok_at(fs, tp), own_s.at[0]),
        pltpu.make_async_copy(sc_in, sc.at[fs], own_s.at[1]),
    ]
    for copy in own:
        copy.start()

    barrier = pltpu.get_barrier_semaphore()
    for o in range(n):
        for x in range(tps):
            if o or x:
                pl.semaphore_signal(
                    barrier, inc=1, device_id=at(grp, turn(fs, o, n), turn(tp, x, tps)), device_id_type=MESH
                )
    for y in range(1, groups):
        pl.semaphore_signal(barrier, inc=1, device_id=at(turn(grp, y, groups), fs, tp), device_id_type=MESH)
    pl.semaphore_wait(barrier, n * tps - 1 + groups - 1)

    def line_block(i, f, share):
        if i == 0:
            return tok_at(f, tp)
        if i == 1:
            return sc.at[f]
        rows = srcs[i + 1].shape[1]
        return outs[i + 1].at[0, span(f * groups + share, rows // groups), :]

    def line_source(i):
        if i < 2:
            return line_block(i, fs, grp)
        return srcs[i + 1].at[0, span(grp, srcs[i + 1].shape[1] // groups), :]

    def line_send(i, zs, up, source=None):
        block = line_block(i, zs * 2 + c, grp)
        there = turn(z, 1 if up else -1, chips) * 2 + c
        return remote(
            block if source is None else source, block, lz_s.at[i, up, zs], lz_r.at[i, zs], at(grp, there, tp)
        )

    def x_block(f, v):
        return tok_at(f, turn(tp, -v, tps))

    def x_send(zs, x):
        block = tok_at(zs * 2 + c, tp)
        return remote(block, block, lx_s.at[x - 1, zs], lx_r.at[x - 1, zs], at(grp, fs, turn(tp, x, tps)))

    def y_send(i, zs, y):
        block = line_block(i, zs * 2 + c, grp)
        return remote(
            block, block, ly_s.at[i - 2, y - 1, zs], ly_r.at[i - 2, y - 1, zs], at(turn(grp, y, groups), fs, tp)
        )

    def sib_block(i, f, v):
        return x_block(f, v) if i == 0 else line_block(i, f, turn(grp, -v, groups))

    def sib_send(i, zs, v, source=None):
        block = sib_block(i, zs * 2 + c, v)
        return remote(
            block if source is None else source, block, ls_s.at[i, v, zs], ls_r.at[i, v, zs], at(grp, both, tp)
        )

    def ways(i):
        return (tps, 1, groups, groups)[i]

    def own_share(i, v):
        if i < 2:
            return None
        return srcs[i + 1].at[0, span(turn(grp, -v, groups), srcs[i + 1].shape[1] // groups), :]

    def ends(up):
        return z < chips - 1 if up else z > 0

    def line_own(i):
        for up in (0, 1):
            @pl.when(ends(up))
            def _():
                line_send(i, z, up, line_source(i)).start()

    def line_spread(i, zs):
        if i == 0:
            for x in range(1, tps):
                x_send(zs, x).start()
        sib_send(i, zs, 0).start()
        if i > 1:
            for y in range(1, groups):
                y_send(i, zs, y).start()

    def line_arrivals(i, d):
        for up in (1, 0):
            zs = turn(z, -d if up else d, chips)

            @pl.when(z >= d if up else z + d < chips)
            def _():
                arrived(line_block(i, zs * 2 + c, grp), lz_r.at[i, zs])

                @pl.when(ends(up))
                def _():
                    line_send(i, zs, up).start()

                line_spread(i, zs)

    def held(k):
        return outs[k].shape[0]

    def e_src(k, f, share):
        first = f * held(k)
        if k < 2:
            rows = srcs[k].shape[1]
            at_rows = pl.ds(0, rows) if share is None else span(share, rows // groups)
            return srcs[k].at[pl.ds(first, held(k)), at_rows, :]
        wide = srcs[k].shape[2]
        at_cols = pl.ds(0, wide) if share is None else span(share, wide // groups)
        return srcs[k].at[pl.ds(first, held(k)), :, at_cols]

    def down_block(k, f, x, share):
        rows, wide = srcs[k].shape[1:]
        at_cols = span(x, wide) if share is None else span(x * groups + share, wide // groups)
        return outs[k].at[:, span(lax.rem(f, band), rows), at_cols]

    def e_dst(k, f, x, share):
        if k == 2:
            return down_block(k, f, x, share)
        rows = srcs[k].shape[1]
        at_rows = span(f, rows) if share is None else span(f * groups + share, rows // groups)
        return outs[k].at[:, at_rows, :]

    def e_slot(k, f, x):
        return f if k < 2 else lax.rem(f, band) * tps + x

    def e_send(k, f, share):
        return remote(
            e_src(k, f, share), e_dst(k, fs, tp, share), e_s.at[k, f], e_r.at[k, e_slot(k, fs, tp)],
            at(grp, f, tp if k < 2 else home),
        )

    def e_pass(k, f, x, y):
        block = e_dst(k, f, x, grp)
        slot = e_slot(k, f, x)
        return remote(block, block, p_s.at[k, slot, y - 1], p_r.at[k, slot, y - 1], at(turn(grp, y, groups), fs, tp))

    def far(s):
        low = (z < chips // 2).astype(jnp.int32)
        down = chips - 1 - s
        down = down - (down <= z).astype(jnp.int32)
        upto = s + (s >= z).astype(jnp.int32)
        return low * down + (1 - low) * upto

    def e_arrive(k, f, x, local):
        def take(share):
            block = e_dst(k, f, x, share)
            arrived(block, e_r.at[k, e_slot(k, f, x)])

        if local:
            take(None)
            return
        take(grp)
        for y in range(1, groups):
            e_pass(k, f, x, y).start()

    def e_settle(k, f, x):
        for y in range(1, groups):
            e_pass(k, f, x, y).wait_send()
            arrived(e_dst(k, f, x, turn(grp, -y, groups)), p_r.at[k, e_slot(k, f, x), y - 1])

    def sd_send(zd, share):
        src = srcs[5].at[:, :, :] if share is None else srcs[5].at[:, :, span(share, srcs[5].shape[2] // groups)]
        return remote(
            src, down_block(5, fs, tp, share), d_s.at[zd], d_r.at[lax.rem(z, half), tp], at(grp, zd * 2 + c, home)
        )

    def sd_pass(q, x, y):
        block = down_block(5, (tp * half + q) * 2 + c, x, grp)
        return remote(
            block, block, dy_s.at[q, x, y - 1], dy_r.at[q, x, y - 1], at(turn(grp, y, groups), fs, tp)
        )

    def sd_sib(q, x, v, local, source=None):
        share = None if local else turn(grp, -v, groups)
        block = down_block(5, (tp * half + q) * 2 + c, x, share)
        return remote(
            block if source is None else source, block, ds_s.at[q, x, v], ds_r.at[q, x, v], at(grp, both, tp)
        )

    for copy in own:
        copy.wait()
    for i in (0, 1, 2, 3):
        line_own(i)
    for s in range(chips - 1):
        for k in (0, 1):
            for dc in (0, 1):
                e_send(k, far(s) * 2 + dc, grp).start()
    for k in (0, 1):
        e_send(k, both, None).start()
    for x in range(1, tps):
        x_send(z, x).start()
    for i in (0, 1, 2, 3):
        for v in range(ways(i)):
            if i or not v:
                sib_send(i, z, v, own_share(i, v)).start()

    @pl.when(home == tp)
    def _():
        e_send(2, both, None).start()
        sd_sib(lax.rem(z, half), tp, 0, True, srcs[5].at[:, :, :]).start()

    @pl.when(home != tp)
    def _():
        for dc in (0, 1):
            e_send(2, z * 2 + dc, None).start()
        sd_send(z, None).start()

    for i in (0, 1, 2, 3):
        line_arrivals(i, 1)
    for s in range(chips - 1):
        for dc in (0, 1):
            e_send(2, far(s) * 2 + dc, grp).start()
        sd_send(far(s), grp).start()

    def keep(k, x):
        rows, wide = srcs[k].shape[1:]
        first = fs * held(k) if k < 3 else 0
        for j in range(held(k)):
            if k in (2, 5):
                outs[k][j, span(lax.rem(fs, band), rows), span(x, wide)] = srcs[k][first + j]
            else:
                outs[k][j, span(fs, rows), :] = srcs[k][first + j]

    for k in (0, 1, 3, 4):
        keep(k, tp)

    @pl.when(home == tp)
    def _():
        keep(2, tp)
        keep(5, tp)

    for k in (0, 1):
        for s in range(chips - 1):
            for dc in (0, 1):
                e_arrive(k, far(s) * 2 + dc, tp, False)
    for d in range(2, chips):
        for i in (0, 1, 2, 3):
            line_arrivals(i, d)

    def sd_sources():
        for q in range(half):
            for x in range(tps):
                yield q, x, tp * half + q

    def downs(k):
        for q, x, zs in sd_sources():
            near = zs == z
            cores = (0, 1) if k == 2 else (0,)
            for dc in cores:
                f = zs * 2 + (dc if k == 2 else c)
                yield q, x, near, f

    for q, x, near, f in downs(2):
        @pl.when(jnp.logical_not(near))
        def _():
            e_arrive(2, f, x, False)

        @pl.when(jnp.logical_and(near, jnp.logical_or(f != fs, tp != x)))
        def _():
            e_arrive(2, f, x, True)

    for q, x, near, f in downs(5):
        @pl.when(jnp.logical_not(near))
        def _():
            arrived(down_block(5, f, x, grp), d_r.at[q, x])
            sd_sib(q, x, 0, False).start()
            for y in range(1, groups):
                sd_pass(q, x, y).start()

        @pl.when(jnp.logical_and(near, tp != x))
        def _():
            arrived(down_block(5, f, x, None), d_r.at[q, x])
            sd_sib(q, x, 0, True).start()

    for zs in range(chips):
        for x in range(1, tps):
            arrived(x_block(zs * 2 + c, x), lx_r.at[x - 1, zs])
            sib_send(0, zs, x).start()
    for dz in range(1, chips):
        zs = turn(z, dz, chips)
        for i in (2, 3):
            for y in range(1, groups):
                arrived(sib_block(i, zs * 2 + c, y), ly_r.at[i - 2, y - 1, zs])
                sib_send(i, zs, y).start()
    for q, x, near, f in downs(5):
        @pl.when(jnp.logical_not(near))
        def _():
            for y in range(1, groups):
                arrived(down_block(5, f, x, turn(grp, -y, groups)), dy_r.at[q, x, y - 1])
                sd_sib(q, x, y, False).start()

    for k in (0, 1):
        arrived(e_dst(k, both, tp, None), e_r.at[k, e_slot(k, both, tp)])
        for s in range(chips - 1):
            for dc in (0, 1):
                e_settle(k, far(s) * 2 + dc, tp)
    for q, x, near, f in downs(2):
        @pl.when(jnp.logical_not(near))
        def _():
            e_settle(2, f, x)
    for zs in range(chips):
        for i in (0, 1, 2, 3):
            for v in range(ways(i)):
                arrived(sib_block(i, zs * 2 + 1 - c, v), ls_r.at[i, v, zs])
    for q, x, near, f in downs(5):
        other = f + 1 - 2 * c
        @pl.when(near)
        def _():
            arrived(down_block(5, other, x, None), ds_r.at[q, x, 0])

        @pl.when(jnp.logical_not(near))
        def _():
            for v in range(groups):
                arrived(down_block(5, other, x, turn(grp, -v, groups)), ds_r.at[q, x, v])

    for zs in range(chips):
        for i in (0, 1, 2, 3):
            for v in range(ways(i)):
                sib_send(i, zs, v).wait_send()
        for x in range(1, tps):
            x_send(zs, x).wait_send()
    for dz in range(1, chips):
        for i in (2, 3):
            for y in range(1, groups):
                y_send(i, turn(z, dz, chips), y).wait_send()
    for d in range(chips):
        for up in (0, 1):
            @pl.when(jnp.logical_and(ends(up), z >= d if up else z + d < chips))
            def _():
                for i in (0, 1, 2, 3):
                    line_send(i, turn(z, -d if up else d, chips), up).wait_send()
    for k in (0, 1):
        e_send(k, both, None).wait_send()
    for s in range(chips - 1):
        for k in (0, 1, 2):
            for dc in (0, 1):
                e_send(k, far(s) * 2 + dc, grp).wait_send()
        sd_send(far(s), grp).wait_send()

    @pl.when(home == tp)
    def _():
        e_send(2, both, None).wait_send()

    @pl.when(home != tp)
    def _():
        for dc in (0, 1):
            e_send(2, z * 2 + dc, None).wait_send()
        sd_send(z, None).wait_send()

    for q, x, near, f in downs(5):
        @pl.when(near)
        def _():
            sd_sib(q, x, 0, True).wait_send()

        @pl.when(jnp.logical_not(near))
        def _():
            for v in range(groups):
                sd_sib(q, x, v, False).wait_send()
            for y in range(1, groups):
                sd_pass(q, x, y).wait_send()


def move(sizes, tokens, scales, gate, up, down, shared_gate, shared_up, shared_down):
    groups, n, tps = sizes
    chips = n // 2
    half = n // tps // 2
    held = gate.shape[0] // n
    bf16 = jnp.bfloat16
    ways = max(groups, tps)

    def rows(a, lead):
        return jax.ShapeDtypeStruct((lead, n * a.shape[1], a.shape[2]), bf16)

    def downs(a, lead):
        return jax.ShapeDtypeStruct((lead, n // tps * a.shape[1], tps * a.shape[2]), bf16)

    dma = pltpu.SemaphoreType.DMA
    return pl.pallas_call(
        functools.partial(move_kernel, sizes),
        out_shape=(
            jax.ShapeDtypeStruct((n, tokens.shape[0], tps * tokens.shape[1]), bf16),
            jax.ShapeDtypeStruct((n,) + scales.shape, jnp.float32),
            rows(gate, held), rows(up, held), downs(down, held),
            rows(shared_gate, 1), rows(shared_up, 1), downs(shared_down, 1),
        ),
        in_specs=[pl.BlockSpec(memory_space=pl.ANY)] * 2 + [pl.BlockSpec(memory_space=pltpu.VMEM)] * 6,
        out_specs=[pl.BlockSpec(memory_space=pltpu.VMEM)] * 8,
        scratch_shapes=[
            dma((2,)), dma((4, 2, chips)), dma((4, chips)), dma((4, ways, chips)), dma((4, ways, chips)),
            dma((tps - 1, chips)), dma((tps - 1, chips)), dma((2, groups - 1, chips)), dma((2, groups - 1, chips)),
            dma((3, n)), dma((3, n)), dma((3, n, groups - 1)), dma((3, n, groups - 1)),
            dma((chips,)), dma((half, tps)), dma((half, tps, groups - 1)), dma((half, tps, groups - 1)),
            dma((half, tps, groups)), dma((half, tps, groups)),
        ],
        compiler_params=pltpu.CompilerParams(
            collective_id=0, has_side_effects=True, vmem_limit_bytes=60 * 1024 * 1024
        ),
        cost_estimate=pl.CostEstimate(flops=400_000_000, bytes_accessed=20_000_000, transcendentals=0),
    )(tokens, scales, gate, up, down, shared_gate, shared_up, shared_down)


def combine_kernel(sizes, part, shared, out, near, held, across, summed, far, local_sem, near_s, near_r, x_s, x_r, z_s, z_r):
    _, n, tps = sizes
    chips = n // 2
    grp, fs, tp = lax.axis_index("grp"), lax.axis_index("fs"), lax.axis_index("tp")
    chip, core = fs // 2, lax.rem(fs, 2)
    rows, cols = out.shape
    f32 = jnp.float32
    step = 32

    def sibling():
        return {"grp": grp, "fs": chip * 2 + 1 - core, "tp": tp}

    def x_peer(x):
        return {"grp": grp, "fs": fs, "tp": lax.rem(tp + x, tps)}

    def z_peer(o):
        return {"grp": grp, "fs": lax.rem(chip + o, chips) * 2 + core, "tp": tp}

    barrier = pltpu.get_barrier_semaphore()
    peers = [sibling()] + [x_peer(x) for x in range(1, tps)] + [z_peer(o) for o in range(1, chips)]
    for peer in peers:
        pl.semaphore_signal(barrier, inc=1, device_id=peer, device_id_type=MESH)
    pl.semaphore_wait(barrier, len(peers))

    def near_copy(o):
        return pltpu.make_async_remote_copy(
            src_ref=part.at[lax.rem(chip + o, chips) * 2 + 1 - core], dst_ref=near.at[o],
            send_sem=near_s.at[o], recv_sem=near_r.at[o], device_id=sibling(), device_id_type=MESH,
        )

    def keep_copy(o):
        return pltpu.make_async_copy(part.at[lax.rem(chip + o, chips) * 2 + core], held.at[o], local_sem.at[o])

    def x_copy(o, x):
        there = pl.multiple_of(lax.rem(tp + x, tps) * cols, cols)
        return pltpu.make_async_remote_copy(
            src_ref=held.at[o, :, pl.ds(there, cols)], dst_ref=across.at[x - 1, o],
            send_sem=x_s.at[x - 1, o], recv_sem=x_r.at[x - 1, o], device_id=x_peer(x), device_id_type=MESH,
        )

    def z_copy(o):
        return pltpu.make_async_remote_copy(
            src_ref=summed.at[o], dst_ref=far.at[o], send_sem=z_s.at[o], recv_sem=z_r.at[o],
            device_id=z_peer(o), device_id_type=MESH,
        )

    order = list(range(1, chips)) + [0]
    for o in order:
        near_copy(o).start()
        keep_copy(o).start()
    for o in order:
        near_copy(o).wait_recv()
        keep_copy(o).wait()

        @pl.loop(0, rows // step)
        def _(i):
            r = pl.ds(pl.multiple_of(i * step, step), step)
            total = held[o, r, :].astype(f32) + near[o, r, :].astype(f32)
            if o == 0:
                total = total + shared[r, :]
            held[o, r, :] = total.astype(jnp.bfloat16)

        for x in range(1, tps):
            x_copy(o, x).start()
    here = pl.ds(pl.multiple_of(tp * cols, cols), cols)
    for o in order:
        for x in range(1, tps):
            x_copy(o, x).wait_recv()

        @pl.loop(0, rows // step)
        def _(i):
            r = pl.ds(pl.multiple_of(i * step, step), step)
            total = held[o, r, here].astype(f32)
            for x in range(1, tps):
                total = total + across[x - 1, o, r, :].astype(f32)
            summed[o, r, :] = total.astype(jnp.bfloat16)

        if o:
            z_copy(o).start()
    for o in range(1, chips):
        z_copy(o).wait_recv()

    @pl.loop(0, rows // step)
    def _(i):
        r = pl.ds(pl.multiple_of(i * step, step), step)
        total = summed[0, r, :].astype(f32)
        for o in range(1, chips):
            total = total + far[o, r, :].astype(f32)
        out[r, :] = total.astype(jnp.bfloat16)

    for o in order:
        near_copy(o).wait_send()
        for x in range(1, tps):
            x_copy(o, x).wait_send()
        if o:
            z_copy(o).wait_send()


def combine(sizes, partial, shared_part):
    _, n, tps = sizes
    chips = n // 2
    rows, width = shared_part.shape
    cols = width // tps
    bf16 = jnp.bfloat16
    dma = pltpu.SemaphoreType.DMA
    return pl.pallas_call(
        functools.partial(combine_kernel, sizes),
        out_shape=jax.ShapeDtypeStruct((rows, cols), bf16),
        in_specs=[pl.BlockSpec(memory_space=pl.ANY), pl.BlockSpec(memory_space=pltpu.VMEM)],
        out_specs=pl.BlockSpec(memory_space=pltpu.VMEM),
        scratch_shapes=[
            pltpu.VMEM((chips, rows, width), bf16),
            pltpu.VMEM((chips, rows, width), bf16),
            pltpu.VMEM((tps - 1, chips, rows, cols), bf16),
            pltpu.VMEM((chips, rows, cols), bf16),
            pltpu.VMEM((chips, rows, cols), bf16),
            dma((chips,)), dma((chips,)), dma((chips,)),
            dma((tps - 1, chips)), dma((tps - 1, chips)), dma((chips,)), dma((chips,)),
        ],
        compiler_params=pltpu.CompilerParams(
            collective_id=1, has_side_effects=True, vmem_limit_bytes=min(60, 8 + 16 * chips * rows * width // 2**20 // 2) * 2**20
        ),
        cost_estimate=pl.CostEstimate(flops=200_000_000, bytes_accessed=20_000_000, transcendentals=0),
    )(partial.reshape(n, rows, width), shared_part)


def per_device(
    sizes,
    tokens,
    routes,
    route_weights,
    norm_gain,
    gate_experts,
    up_experts,
    down_experts,
    shared_gate,
    shared_up,
    shared_down,
):
    bf16, f32 = jnp.bfloat16, jnp.float32
    groups, n, tps = sizes
    width = tokens.shape[1] * tps
    experts_all = gate_experts.shape[0]
    held = experts_all // n
    gain_rows = norm_gain[None, :, None]
    chosen = routes[:, :, None] == jnp.arange(experts_all, dtype=jnp.int32)[None, None, :]
    per_expert = jnp.sum(jnp.where(chosen, route_weights[:, :, None], 0.0), axis=1)
    count = tokens.shape[0]
    scales = jnp.pad(per_expert.T, ((0, 0), (0, -count % 128)))
    moved = move(
        sizes,
        tokens,
        scales,
        (gate_experts * gain_rows).astype(bf16),
        (up_experts * gain_rows).astype(bf16),
        down_experts.astype(bf16),
        (shared_gate[None] * gain_rows).astype(bf16),
        (shared_up[None] * gain_rows).astype(bf16),
        shared_down[None].astype(bf16),
    )
    everyone, scales, gate_local, up_local, down_local, sg, su, sd = moved
    sg, su, sd = sg[0], su[0], sd[0]
    here = lax.axis_index("fs")
    widened = everyone.reshape(n * count, width).astype(f32)
    rows = (widened * lax.rsqrt(jnp.mean(widened * widened, axis=1, keepdims=True) + 1e-06)).astype(bf16)
    normed = lax.dynamic_slice_in_dim(rows, here * count, count, 0)
    scale = lax.dynamic_slice_in_dim(scales, here * held, held, 1)[:, :, :count]
    scale = scale.transpose(0, 2, 1).reshape(n * count, held)

    def hidden(x, g, u):
        return jax.nn.silu(jnp.dot(x, g, preferred_element_type=f32)) * jnp.dot(x, u, preferred_element_type=f32)

    active = jnp.concatenate(
        [(hidden(rows, gate_local[j], up_local[j]) * scale[:, j:j + 1]).astype(bf16) for j in range(held)], axis=1
    )
    partial = jnp.dot(active, down_local.reshape(-1, width), preferred_element_type=f32).astype(bf16)
    shared_part = jnp.dot(hidden(normed, sg, su).astype(bf16), sd, preferred_element_type=f32)
    mixed = combine(sizes, partial, shared_part)
    return mixed, gate_local, up_local, down_local, sg, su, sd


def solution(mesh):
    sizes = (mesh.shape["grp"], mesh.shape["fs"], mesh.shape["tp"])
    return jax.shard_map(
        functools.partial(per_device, sizes),
        mesh=mesh,
        in_specs=(
            P(("grp", "fs"), "tp"),
            P(("grp", "fs"), None),
            P(("grp", "fs"), None),
            P("fs"),
            P(None, "fs", "tp"),
            P(None, "fs", "tp"),
            P(None, "fs", "tp"),
            P("fs", "tp"),
            P("fs", "tp"),
            P("fs", "tp"),
        ),
        out_specs=(
            P(("grp", "fs"), "tp"),
            P(("grp", "fs"), None, "tp"),
            P(("grp", "fs"), None, "tp"),
            P(("grp", "fs"), "tp", None),
            P("grp", "tp"),
            P("grp", "tp"),
            P(("grp", "tp"), None),
        ),
        check_vma=False,
    )
```

```python
import functools
import math
from types import SimpleNamespace

import jax
import jax.numpy as jnp
from jax import lax
from jax.experimental import pallas as pl
from jax.experimental.pallas import tpu as pltpu
from jax.sharding import PartitionSpec as P

MESH = pl.DeviceIdType.MESH


def plan(sizes, tok_in, sc_in, srcs, tok, sc, outs, sems):
    groups, n, tps = sizes
    chips, band = n // 2, n // tps
    half = band // 2
    (
        own_s, lz_s, lz_r, ls_s, ls_r, lx_s, lx_r, ly_s, ly_r,
        e_s, e_r, p_s, p_r, d_s, d_r, dy_s, dy_r, ds_s, ds_r,
    ) = sems
    grp, fs, tp = lax.axis_index("grp"), lax.axis_index("fs"), lax.axis_index("tp")
    z, c = fs // 2, lax.rem(fs, 2)
    home = fs // band
    cols = tok_in.shape[1]
    both = fs + 1 - 2 * c

    def at(g, f, t):
        return {"grp": g, "fs": f, "tp": t}

    def turn(v, by, size):
        return lax.rem(v + by + size, size)

    def remote(src, dst, ssem, rsem, where):
        return pltpu.make_async_remote_copy(
            src_ref=src, dst_ref=dst, send_sem=ssem, recv_sem=rsem, device_id=where, device_id_type=MESH
        )

    def arrived(block, rsem):
        remote(block, block, rsem, rsem, at(grp, both, tp)).wait_recv()

    def span(start, size):
        return pl.ds(pl.multiple_of(start * size, size), size)

    def tok_at(f, x):
        return tok.at[f, :, span(x, cols)]

    own = [
        pltpu.make_async_copy(tok_in, tok_at(fs, tp), own_s.at[0]),
        pltpu.make_async_copy(sc_in, sc.at[fs], own_s.at[1]),
    ]
    for copy in own:
        copy.start()

    barrier = pltpu.get_barrier_semaphore()
    for o in range(n):
        for x in range(tps):
            if o or x:
                pl.semaphore_signal(
                    barrier, inc=1, device_id=at(grp, turn(fs, o, n), turn(tp, x, tps)), device_id_type=MESH
                )
    for y in range(1, groups):
        pl.semaphore_signal(barrier, inc=1, device_id=at(turn(grp, y, groups), fs, tp), device_id_type=MESH)
    pl.semaphore_wait(barrier, n * tps - 1 + groups - 1)

    def line_block(i, f, share):
        if i == 0:
            return tok_at(f, tp)
        if i == 1:
            return sc.at[f]
        rows = srcs[i + 1].shape[1]
        return outs[i + 1].at[0, span(f * groups + share, rows // groups), :]

    def line_source(i):
        if i < 2:
            return line_block(i, fs, grp)
        return srcs[i + 1].at[0, span(grp, srcs[i + 1].shape[1] // groups), :]

    def line_send(i, zs, up, source=None):
        block = line_block(i, zs * 2 + c, grp)
        there = turn(z, 1 if up else -1, chips) * 2 + c
        return remote(
            block if source is None else source, block, lz_s.at[i, up, zs], lz_r.at[i, zs], at(grp, there, tp)
        )

    def x_block(f, v):
        return tok_at(f, turn(tp, -v, tps))

    def x_send(zs, x):
        block = tok_at(zs * 2 + c, tp)
        return remote(block, block, lx_s.at[x - 1, zs], lx_r.at[x - 1, zs], at(grp, fs, turn(tp, x, tps)))

    def y_send(i, zs, y):
        block = line_block(i, zs * 2 + c, grp)
        return remote(
            block, block, ly_s.at[i - 2, y - 1, zs], ly_r.at[i - 2, y - 1, zs], at(turn(grp, y, groups), fs, tp)
        )

    def sib_block(i, f, v):
        return x_block(f, v) if i == 0 else line_block(i, f, turn(grp, -v, groups))

    def sib_send(i, zs, v, source=None):
        block = sib_block(i, zs * 2 + c, v)
        return remote(
            block if source is None else source, block, ls_s.at[i, v, zs], ls_r.at[i, v, zs], at(grp, both, tp)
        )

    def ways(i):
        return (tps, 1, groups, groups)[i]

    def own_share(i, v):
        if i < 2:
            return None
        return srcs[i + 1].at[0, span(turn(grp, -v, groups), srcs[i + 1].shape[1] // groups), :]

    def ends(up):
        return z < chips - 1 if up else z > 0

    def line_own(i):
        for up in (0, 1):
            @pl.when(ends(up))
            def _():
                line_send(i, z, up, line_source(i)).start()

    def line_spread(i, zs):
        if i == 0:
            for x in range(1, tps):
                x_send(zs, x).start()
        sib_send(i, zs, 0).start()
        if i > 1:
            for y in range(1, groups):
                y_send(i, zs, y).start()

    def line_arrivals(i, d):
        for up in (1, 0):
            zs = turn(z, -d if up else d, chips)

            @pl.when(z >= d if up else z + d < chips)
            def _():
                arrived(line_block(i, zs * 2 + c, grp), lz_r.at[i, zs])

                @pl.when(ends(up))
                def _():
                    line_send(i, zs, up).start()

                line_spread(i, zs)

    def held(k):
        return outs[k].shape[0]

    def e_src(k, f, share):
        first = f * held(k)
        if k < 2:
            rows = srcs[k].shape[1]
            at_rows = pl.ds(0, rows) if share is None else span(share, rows // groups)
            return srcs[k].at[pl.ds(first, held(k)), at_rows, :]
        wide = srcs[k].shape[2]
        at_cols = pl.ds(0, wide) if share is None else span(share, wide // groups)
        return srcs[k].at[pl.ds(first, held(k)), :, at_cols]

    def down_block(k, f, x, share):
        rows, wide = srcs[k].shape[1:]
        at_cols = span(x, wide) if share is None else span(x * groups + share, wide // groups)
        return outs[k].at[:, span(lax.rem(f, band), rows), at_cols]

    def e_dst(k, f, x, share):
        if k == 2:
            return down_block(k, f, x, share)
        rows = srcs[k].shape[1]
        at_rows = span(f, rows) if share is None else span(f * groups + share, rows // groups)
        return outs[k].at[:, at_rows, :]

    def e_slot(k, f, x):
        return f if k < 2 else lax.rem(f, band) * tps + x

    def e_send(k, f, share):
        return remote(
            e_src(k, f, share), e_dst(k, fs, tp, share), e_s.at[k, f], e_r.at[k, e_slot(k, fs, tp)],
            at(grp, f, tp if k < 2 else home),
        )

    def e_pass(k, f, x, y):
        block = e_dst(k, f, x, grp)
        slot = e_slot(k, f, x)
        return remote(block, block, p_s.at[k, slot, y - 1], p_r.at[k, slot, y - 1], at(turn(grp, y, groups), fs, tp))

    def far(s):
        low = (z < chips // 2).astype(jnp.int32)
        down = chips - 1 - s
        down = down - (down <= z).astype(jnp.int32)
        upto = s + (s >= z).astype(jnp.int32)
        return low * down + (1 - low) * upto

    def e_arrive(k, f, x, local):
        def take(share):
            block = e_dst(k, f, x, share)
            arrived(block, e_r.at[k, e_slot(k, f, x)])

        if local:
            take(None)
            return
        take(grp)
        for y in range(1, groups):
            e_pass(k, f, x, y).start()

    def e_settle(k, f, x):
        for y in range(1, groups):
            e_pass(k, f, x, y).wait_send()
            arrived(e_dst(k, f, x, turn(grp, -y, groups)), p_r.at[k, e_slot(k, f, x), y - 1])

    def sd_send(zd, share):
        src = srcs[5].at[:, :, :] if share is None else srcs[5].at[:, :, span(share, srcs[5].shape[2] // groups)]
        return remote(
            src, down_block(5, fs, tp, share), d_s.at[zd], d_r.at[lax.rem(z, half), tp], at(grp, zd * 2 + c, home)
        )

    def sd_pass(q, x, y):
        block = down_block(5, (tp * half + q) * 2 + c, x, grp)
        return remote(
            block, block, dy_s.at[q, x, y - 1], dy_r.at[q, x, y - 1], at(turn(grp, y, groups), fs, tp)
        )

    def sd_sib(q, x, v, local, source=None):
        share = None if local else turn(grp, -v, groups)
        block = down_block(5, (tp * half + q) * 2 + c, x, share)
        return remote(
            block if source is None else source, block, ds_s.at[q, x, v], ds_r.at[q, x, v], at(grp, both, tp)
        )


    def sd_sources():
        for q in range(half):
            for x in range(tps):
                yield q, x, tp * half + q

    def downs(k):
        for q, x, zs in sd_sources():
            for dc in (0, 1) if k == 2 else (c,):
                yield q, x, zs == z, zs * 2 + dc

    def keep(k, x):
        rows, wide = srcs[k].shape[1:]
        first = fs * held(k) if k < 3 else 0
        for j in range(held(k)):
            if k in (2, 5):
                outs[k][j, span(lax.rem(fs, band), rows), span(x, wide)] = srcs[k][first + j]
            else:
                outs[k][j, span(fs, rows), :] = srcs[k][first + j]

    def keep_all():
        for k in (0, 1, 3, 4):
            keep(k, tp)

        @pl.when(home == tp)
        def _():
            keep(2, tp)
            keep(5, tp)

    def near_sends(lines):
        for k in (0, 1):
            e_send(k, both, None).start()
        for x in range(1, tps):
            x_send(z, x).start()
        for i in lines:
            for v in range(ways(i)):
                if i or not v:
                    sib_send(i, z, v, own_share(i, v)).start()

    def near_downs():
        @pl.when(home == tp)
        def _():
            e_send(2, both, None).start()
            sd_sib(lax.rem(z, half), tp, 0, True, srcs[5].at[:, :, :]).start()

        @pl.when(home != tp)
        def _():
            for dc in (0, 1):
                e_send(2, z * 2 + dc, None).start()
            sd_send(z, None).start()

    def rows_out(s):
        for k in (0, 1):
            for dc in (0, 1):
                e_send(k, far(s) * 2 + dc, grp).start()

    def rows_in(s):
        for dc in (0, 1):
            for k in (0, 1):
                e_arrive(k, far(s) * 2 + dc, tp, False)

    def downs_out():
        for s in range(chips - 1):
            for dc in (0, 1):
                e_send(2, far(s) * 2 + dc, grp).start()

    def sds_out():
        for s in range(chips - 1):
            sd_send(far(s), grp).start()

    def downs_in(want):
        for q, x, near, f in downs(2):
            if q * tps + x not in want:
                continue

            @pl.when(jnp.logical_not(near))
            def _():
                e_arrive(2, f, x, False)

            @pl.when(jnp.logical_and(near, jnp.logical_or(f != fs, tp != x)))
            def _():
                e_arrive(2, f, x, True)

    def sds_in():
        for q, x, near, f in downs(5):
            @pl.when(jnp.logical_not(near))
            def _():
                arrived(down_block(5, f, x, grp), d_r.at[q, x])
                sd_sib(q, x, 0, False).start()
                for y in range(1, groups):
                    sd_pass(q, x, y).start()

            @pl.when(jnp.logical_and(near, tp != x))
            def _():
                arrived(down_block(5, f, x, None), d_r.at[q, x])
                sd_sib(q, x, 0, True).start()

    def x_in(zs):
        for x in range(1, tps):
            arrived(x_block(zs * 2 + c, x), lx_r.at[x - 1, zs])
            sib_send(0, zs, x).start()

    def x_arrivals(d):
        if not d:
            x_in(z)
            return
        for up in (1, 0):
            @pl.when(z >= d if up else z + d < chips)
            def _():
                x_in(turn(z, -d if up else d, chips))

    def shared_y():
        for dz in range(1, chips):
            zs = turn(z, dz, chips)
            for i in (2, 3):
                for y in range(1, groups):
                    arrived(sib_block(i, zs * 2 + c, y), ly_r.at[i - 2, y - 1, zs])
                    sib_send(i, zs, y).start()
        for q, x, near, f in downs(5):
            @pl.when(jnp.logical_not(near))
            def _():
                for y in range(1, groups):
                    arrived(down_block(5, f, x, turn(grp, -y, groups)), dy_r.at[q, x, y - 1])
                    sd_sib(q, x, y, False).start()

    def rows_settled():
        for k in (0, 1):
            arrived(e_dst(k, both, tp, None), e_r.at[k, e_slot(k, both, tp)])
            for s in range(chips - 1):
                for dc in (0, 1):
                    e_settle(k, far(s) * 2 + dc, tp)

    def downs_settled():
        for q, x, near, f in downs(2):
            @pl.when(jnp.logical_not(near))
            def _():
                e_settle(2, f, x)

    def line_settled(i):
        for zs in range(chips):
            for v in range(ways(i)):
                arrived(sib_block(i, zs * 2 + 1 - c, v), ls_r.at[i, v, zs])

    def sds_settled():
        for q, x, near, f in downs(5):
            other = f + 1 - 2 * c

            @pl.when(near)
            def _():
                arrived(down_block(5, other, x, None), ds_r.at[q, x, 0])

            @pl.when(jnp.logical_not(near))
            def _():
                for v in range(groups):
                    arrived(down_block(5, other, x, turn(grp, -v, groups)), ds_r.at[q, x, v])

    def sent():
        for zs in range(chips):
            for i in (0, 1, 2, 3):
                for v in range(ways(i)):
                    sib_send(i, zs, v).wait_send()
            for x in range(1, tps):
                x_send(zs, x).wait_send()
        for dz in range(1, chips):
            for i in (2, 3):
                for y in range(1, groups):
                    y_send(i, turn(z, dz, chips), y).wait_send()
        for d in range(chips):
            for up in (0, 1):
                @pl.when(jnp.logical_and(ends(up), z >= d if up else z + d < chips))
                def _():
                    for i in (0, 1, 2, 3):
                        line_send(i, turn(z, -d if up else d, chips), up).wait_send()
        for k in (0, 1):
            e_send(k, both, None).wait_send()
        for s in range(chips - 1):
            for k in (0, 1, 2):
                for dc in (0, 1):
                    e_send(k, far(s) * 2 + dc, grp).wait_send()
            sd_send(far(s), grp).wait_send()

        @pl.when(home == tp)
        def _():
            e_send(2, both, None).wait_send()

        @pl.when(home != tp)
        def _():
            for dc in (0, 1):
                e_send(2, z * 2 + dc, None).wait_send()
            sd_send(z, None).wait_send()

        for q, x, near, f in downs(5):
            @pl.when(near)
            def _():
                sd_sib(q, x, 0, True).wait_send()

            @pl.when(jnp.logical_not(near))
            def _():
                for v in range(groups):
                    sd_sib(q, x, v, False).wait_send()
                for y in range(1, groups):
                    sd_pass(q, x, y).wait_send()

    for copy in own:
        copy.wait()
    return SimpleNamespace(**locals())


def move_kernel(sizes, *refs):
    chips = sizes[1] // 2
    m = plan(sizes, refs[0], refs[1], refs[2:8], refs[8], refs[9], refs[10:16], refs[16:])
    for i in (0, 1):
        m.line_own(i)
    m.rows_out(0)
    m.near_sends((0, 1, 2, 3))
    m.near_downs()
    for d in range(1, chips):
        m.line_arrivals(0, d)
        m.line_arrivals(1, d)
        m.rows_out(d) if d < chips - 1 else None
    m.downs_out()
    for i in (2, 3):
        m.line_own(i)
    m.sds_out()
    m.keep_all()
    for s in range(chips - 1):
        m.rows_in(s)
    for d in range(chips):
        m.x_arrivals(d)
    for d in range(1, chips):
        for i in (2, 3):
            m.line_arrivals(i, d)
    m.downs_in(range(sizes[1]))
    m.sds_in()
    m.shared_y()
    m.rows_settled()
    m.downs_settled()
    for i in (0, 1, 2, 3):
        m.line_settled(i)
    m.sds_settled()
    m.sent()


def fused_kernel(sizes, *refs):
    groups, n, tps = sizes
    chips = n // 2
    bf16, f32 = jnp.bfloat16, jnp.float32
    out, outs = refs[8], refs[9:15]
    tok, sc, nb, act, mine, theirs, near, across, summed, zr, extra, hs = refs[15:27]
    near_s, near_r, x_s, x_r, z_s, z_r = refs[27:33]
    m = plan(sizes, refs[0], refs[1], refs[2:8], tok, sc, outs, refs[33:])
    z, c, tp, fs, grp = m.z, m.c, m.tp, m.fs, m.grp
    gate, up, down, sg, su, sd = outs
    held, _, hid = gate.shape
    count, cols = out.shape
    width = cols * tps

    for i in (0, 1):
        m.line_own(i)
    m.rows_out(0)
    m.near_sends((0, 1))
    m.near_downs()
    for d in range(1, chips):
        m.line_arrivals(0, d)
        m.line_arrivals(1, d)
        if d < chips - 1:
            m.rows_out(d)
        m.x_arrivals(d - 1)
    m.downs_out()
    for i in (2, 3):
        m.line_own(i)
        for v in range(groups):
            m.sib_send(i, z, v, m.own_share(i, v)).start()
    m.sds_out()
    m.keep_all()
    for s in range(chips - 1):
        m.rows_in(s)
    m.x_arrivals(chips - 1)
    m.rows_settled()
    m.line_settled(0)
    m.line_settled(1)

    step = 32

    def norm(f):
        @pl.loop(0, count // step)
        def _(i):
            r = pl.ds(pl.multiple_of(i * step, step), step)
            wide = tok[f, r, :].astype(f32)
            mean = jnp.mean(wide * wide, axis=1, keepdims=True)
            nb[r, :] = (wide * lax.rsqrt(mean + 1e-06)).astype(bf16)

    def hidden(g, u):
        gated = jnp.dot(nb[...], g, preferred_element_type=f32)
        return jax.nn.silu(gated) * jnp.dot(nb[...], u, preferred_element_type=f32)

    def active(f):
        norm(f)
        columns = sc[f].T[:count]
        lane = lax.broadcasted_iota(jnp.int32, columns.shape, 1)
        for j in range(held):
            scale = jnp.sum(jnp.where(lane == fs * held + j, columns, 0.0), axis=1, keepdims=True)
            act[f, :, j * hid:(j + 1) * hid] = (hidden(gate[j], up[j]) * scale).astype(bf16)

    parts = m.half * tps
    for p in range(parts):
        lo, hi = n * p // parts, n * (p + 1) // parts

        @pl.loop(lo, hi)
        def _(f):
            active(f)

        m.downs_in((p,))
    m.downs_settled()

    def goal(s):
        return m.far(s) if s < chips - 1 else z

    chunk = min(512, width)

    def product(f, to, s):
        @pl.loop(0, width // chunk)
        def _(j):
            at_j = m.span(j, chunk)
            total = jnp.dot(act[f, :, :hid], down[0, :, at_j], preferred_element_type=f32)
            for e in range(1, held):
                total = total + jnp.dot(act[f, :, e * hid:(e + 1) * hid], down[e, :, at_j], preferred_element_type=f32)
            to[s, :, at_j] = total.astype(bf16)

    def near_copy(s):
        return m.remote(theirs.at[s], near.at[s], near_s.at[s], near_r.at[s], m.at(grp, m.both, tp))

    def x_copy(s, x):
        there = m.turn(tp, x, tps)
        return m.remote(
            mine.at[s, :, m.span(there, cols)], across.at[x - 1, s], x_s.at[x - 1, s], x_r.at[x - 1, s], m.at(grp, fs, there)
        )

    def z_copy(s, zd, rising):
        there = m.turn(z, 1 if rising else -1, chips) * 2 + c
        return m.remote(
            summed.at[s], zr.at[rising, zd], z_s.at[s], z_r.at[rising, zd], m.at(grp, there, tp)
        )

    def produce(s):
        product(goal(s) * 2 + 1 - c, theirs, s)
        near_copy(s).start()
        product(goal(s) * 2 + c, mine, s)

    def meet(s, extra=None):
        near_copy(s).wait_recv()

        @pl.loop(0, count // step)
        def _(i):
            r = pl.ds(pl.multiple_of(i * step, step), step)
            total = mine[s, r, :].astype(f32) + near[s, r, :].astype(f32)
            if extra is not None:
                total = total + extra[r, :]
            mine[s, r, :] = total.astype(bf16)

        for x in range(1, tps):
            x_copy(s, x).start()

    here = m.span(tp, cols)

    def total_of(s, r):
        total = mine[s, r, here].astype(f32)
        for x in range(1, tps):
            total = total + across[x - 1, s, r, :].astype(f32)
        return total

    def x_met(s):
        for x in range(1, tps):
            x_copy(s, x).wait_recv()

    def onward(s):
        zd = goal(s)
        x_met(s)
        for rising in (1, 0):
            @pl.when(zd > z if rising else zd < z)
            def _():
                behind = z > 0 if rising else z < chips - 1

                @pl.when(behind)
                def _():
                    m.arrived(zr.at[rising, zd], z_r.at[rising, zd])

                    @pl.loop(0, count // step)
                    def _(i):
                        r = pl.ds(pl.multiple_of(i * step, step), step)
                        summed[s, r, :] = (total_of(s, r) + zr[rising, zd, r, :].astype(f32)).astype(bf16)

                @pl.when(jnp.logical_not(behind))
                def _():
                    @pl.loop(0, count // step)
                    def _(i):
                        r = pl.ds(pl.multiple_of(i * step, step), step)
                        summed[s, r, :] = total_of(s, r).astype(bf16)

                z_copy(s, zd, rising).start()

    produce(0)
    for s in range(1, chips):
        produce(s)
        meet(s - 1)

    for d in range(1, chips):
        for i in (2, 3):
            m.line_arrivals(i, d)
    m.sds_in()
    m.shared_y()
    for i in (2, 3):
        m.line_settled(i)
    m.sds_settled()
    norm(fs)
    hs[...] = hidden(sg[0], su[0]).astype(bf16)

    @pl.loop(0, width // chunk)
    def _(j):
        at_j = m.span(j, chunk)
        extra[:, at_j] = jnp.dot(hs[...], sd[0, :, at_j], preferred_element_type=f32)

    meet(chips - 1, extra)
    for s in range(chips - 1):
        onward(s)
    last = chips - 1
    x_met(last)
    for rising in (1, 0):
        @pl.when(z > 0 if rising else z < chips - 1)
        def _():
            m.arrived(zr.at[rising, z], z_r.at[rising, z])

    @pl.loop(0, count // step)
    def _(i):
        r = pl.ds(pl.multiple_of(i * step, step), step)
        extra[r, :cols] = total_of(last, r)

    for rising in (1, 0):
        @pl.when(z > 0 if rising else z < chips - 1)
        def _():
            @pl.loop(0, count // step)
            def _(i):
                r = pl.ds(pl.multiple_of(i * step, step), step)
                extra[r, :cols] = extra[r, :cols] + zr[rising, z, r, :].astype(f32)

    @pl.loop(0, count // step)
    def _(i):
        r = pl.ds(pl.multiple_of(i * step, step), step)
        out[r, :] = extra[r, :cols].astype(bf16)

    for s in range(chips):
        near_copy(s).wait_send()
        for x in range(1, tps):
            x_copy(s, x).wait_send()
        if s < chips - 1:
            zd = goal(s)
            for rising in (1, 0):
                @pl.when(zd > z if rising else zd < z)
                def _():
                    z_copy(s, zd, rising).wait_send()
    m.sent()


def moved_shapes(sizes, gate, up, down, shared_gate, shared_up, shared_down):
    _, n, tps = sizes
    held = gate.shape[0] // n

    def rows(a, lead):
        return jax.ShapeDtypeStruct((lead, n * a.shape[1], a.shape[2]), jnp.bfloat16)

    def downs(a, lead):
        return jax.ShapeDtypeStruct((lead, n // tps * a.shape[1], tps * a.shape[2]), jnp.bfloat16)

    return [
        rows(gate, held), rows(up, held), downs(down, held),
        rows(shared_gate, 1), rows(shared_up, 1), downs(shared_down, 1),
    ]


def plan_sems(sizes):
    groups, n, tps = sizes
    chips, half, ways = n // 2, n // tps // 2, max(groups, tps)
    dma = pltpu.SemaphoreType.DMA
    return [
        dma((2,)), dma((4, 2, chips)), dma((4, chips)), dma((4, ways, chips)), dma((4, ways, chips)),
        dma((tps - 1, chips)), dma((tps - 1, chips)), dma((2, groups - 1, chips)), dma((2, groups - 1, chips)),
        dma((3, n)), dma((3, n)), dma((3, n, groups - 1)), dma((3, n, groups - 1)),
        dma((chips,)), dma((half, tps)), dma((half, tps, groups - 1)), dma((half, tps, groups - 1)),
        dma((half, tps, groups)), dma((half, tps, groups)),
    ]


def token_shapes(sizes, tokens, scales):
    n, tps = sizes[1:]
    return (n, tokens.shape[0], tps * tokens.shape[1]), (n,) + scales.shape


def move(sizes, tokens, scales, *weights):
    tok, sc = token_shapes(sizes, tokens, scales)
    return pl.pallas_call(
        functools.partial(move_kernel, sizes),
        out_shape=[jax.ShapeDtypeStruct(tok, jnp.bfloat16), jax.ShapeDtypeStruct(sc, jnp.float32)]
        + moved_shapes(sizes, *weights),
        in_specs=[pl.BlockSpec(memory_space=pl.ANY)] * 2 + [pl.BlockSpec(memory_space=pltpu.VMEM)] * 6,
        out_specs=[pl.BlockSpec(memory_space=pltpu.VMEM)] * 8,
        scratch_shapes=plan_sems(sizes),
        compiler_params=pltpu.CompilerParams(
            collective_id=0, has_side_effects=True, vmem_limit_bytes=60 * 1024 * 1024
        ),
        cost_estimate=pl.CostEstimate(flops=400_000_000, bytes_accessed=20_000_000, transcendentals=0),
    )(tokens, scales, *weights)


def fused_scratch(sizes, tokens, scales, gate, shared_gate):
    _, n, tps = sizes
    chips = n // 2
    count, cols = tokens.shape
    width = cols * tps
    tok, sc = token_shapes(sizes, tokens, scales)
    held, hid = gate.shape[0] // n, gate.shape[2]
    bf16, f32 = jnp.bfloat16, jnp.float32
    return [
        (tok, bf16), (sc, f32), ((count, width), bf16), ((n, count, held * hid), bf16),
        ((chips, count, width), bf16), ((chips, count, width), bf16), ((chips, count, width), bf16),
        ((tps - 1, chips, count, cols), bf16), ((chips, count, cols), bf16), ((2, chips, count, cols), bf16),
        ((count, width), f32), ((count, shared_gate.shape[2]), bf16),
    ]


def size_of(shape, dtype):
    return math.prod(shape) * jnp.dtype(dtype).itemsize


def fused_fits(sizes, tokens, scales, *weights):
    total = sum(size_of(*s) for s in fused_scratch(sizes, tokens, scales, weights[0], weights[3]))
    total += sum(size_of(s.shape, s.dtype) for s in moved_shapes(sizes, *weights)) + sum(size_of(w.shape, w.dtype) for w in weights)
    return total + 2 * size_of(tokens.shape, tokens.dtype) < 54 * 2**20


def fused(sizes, tokens, scales, *weights):
    _, n, tps = sizes
    chips = n // 2
    dma = pltpu.SemaphoreType.DMA
    return pl.pallas_call(
        functools.partial(fused_kernel, sizes),
        out_shape=[jax.ShapeDtypeStruct(tokens.shape, jnp.bfloat16)] + moved_shapes(sizes, *weights),
        in_specs=[pl.BlockSpec(memory_space=pl.ANY)] * 2 + [pl.BlockSpec(memory_space=pltpu.VMEM)] * 6,
        out_specs=[pl.BlockSpec(memory_space=pltpu.VMEM)] * 7,
        scratch_shapes=[pltpu.VMEM(*s) for s in fused_scratch(sizes, tokens, scales, weights[0], weights[3])]
        + [dma((chips,)), dma((chips,)), dma((tps - 1, chips)), dma((tps - 1, chips)), dma((chips,)), dma((2, chips))]
        + plan_sems(sizes),
        compiler_params=pltpu.CompilerParams(
            collective_id=2, has_side_effects=True, vmem_limit_bytes=60 * 1024 * 1024
        ),
        cost_estimate=pl.CostEstimate(flops=12_000_000_000, bytes_accessed=20_000_000, transcendentals=0),
    )(tokens, scales, *weights)


def combine_kernel(sizes, part, shared, out, near, held, across, summed, far, local_sem, near_s, near_r, x_s, x_r, z_s, z_r):
    _, n, tps = sizes
    chips = n // 2
    grp, fs, tp = lax.axis_index("grp"), lax.axis_index("fs"), lax.axis_index("tp")
    chip, core = fs // 2, lax.rem(fs, 2)
    rows, cols = out.shape
    f32 = jnp.float32
    step = 32

    def sibling():
        return {"grp": grp, "fs": chip * 2 + 1 - core, "tp": tp}

    def x_peer(x):
        return {"grp": grp, "fs": fs, "tp": lax.rem(tp + x, tps)}

    def z_peer(o):
        return {"grp": grp, "fs": lax.rem(chip + o, chips) * 2 + core, "tp": tp}

    barrier = pltpu.get_barrier_semaphore()
    peers = [sibling()] + [x_peer(x) for x in range(1, tps)] + [z_peer(o) for o in range(1, chips)]
    for peer in peers:
        pl.semaphore_signal(barrier, inc=1, device_id=peer, device_id_type=MESH)
    pl.semaphore_wait(barrier, len(peers))

    def near_copy(o):
        return pltpu.make_async_remote_copy(
            src_ref=part.at[lax.rem(chip + o, chips) * 2 + 1 - core], dst_ref=near.at[o],
            send_sem=near_s.at[o], recv_sem=near_r.at[o], device_id=sibling(), device_id_type=MESH,
        )

    def keep_copy(o):
        return pltpu.make_async_copy(part.at[lax.rem(chip + o, chips) * 2 + core], held.at[o], local_sem.at[o])

    def x_copy(o, x):
        there = pl.multiple_of(lax.rem(tp + x, tps) * cols, cols)
        return pltpu.make_async_remote_copy(
            src_ref=held.at[o, :, pl.ds(there, cols)], dst_ref=across.at[x - 1, o],
            send_sem=x_s.at[x - 1, o], recv_sem=x_r.at[x - 1, o], device_id=x_peer(x), device_id_type=MESH,
        )

    def z_copy(o):
        return pltpu.make_async_remote_copy(
            src_ref=summed.at[o], dst_ref=far.at[o], send_sem=z_s.at[o], recv_sem=z_r.at[o],
            device_id=z_peer(o), device_id_type=MESH,
        )

    order = list(range(1, chips)) + [0]
    for o in order:
        near_copy(o).start()
        keep_copy(o).start()
    for o in order:
        near_copy(o).wait_recv()
        keep_copy(o).wait()

        @pl.loop(0, rows // step)
        def _(i):
            r = pl.ds(pl.multiple_of(i * step, step), step)
            total = held[o, r, :].astype(f32) + near[o, r, :].astype(f32)
            if o == 0:
                total = total + shared[r, :]
            held[o, r, :] = total.astype(jnp.bfloat16)

        for x in range(1, tps):
            x_copy(o, x).start()
    here = pl.ds(pl.multiple_of(tp * cols, cols), cols)
    for o in order:
        for x in range(1, tps):
            x_copy(o, x).wait_recv()

        @pl.loop(0, rows // step)
        def _(i):
            r = pl.ds(pl.multiple_of(i * step, step), step)
            total = held[o, r, here].astype(f32)
            for x in range(1, tps):
                total = total + across[x - 1, o, r, :].astype(f32)
            summed[o, r, :] = total.astype(jnp.bfloat16)

        if o:
            z_copy(o).start()
    for o in range(1, chips):
        z_copy(o).wait_recv()

    @pl.loop(0, rows // step)
    def _(i):
        r = pl.ds(pl.multiple_of(i * step, step), step)
        total = summed[0, r, :].astype(f32)
        for o in range(1, chips):
            total = total + far[o, r, :].astype(f32)
        out[r, :] = total.astype(jnp.bfloat16)

    for o in order:
        near_copy(o).wait_send()
        for x in range(1, tps):
            x_copy(o, x).wait_send()
        if o:
            z_copy(o).wait_send()


def combine(sizes, partial, shared_part):
    _, n, tps = sizes
    chips = n // 2
    rows, width = shared_part.shape
    cols = width // tps
    bf16 = jnp.bfloat16
    dma = pltpu.SemaphoreType.DMA
    return pl.pallas_call(
        functools.partial(combine_kernel, sizes),
        out_shape=jax.ShapeDtypeStruct((rows, cols), bf16),
        in_specs=[pl.BlockSpec(memory_space=pl.ANY), pl.BlockSpec(memory_space=pltpu.VMEM)],
        out_specs=pl.BlockSpec(memory_space=pltpu.VMEM),
        scratch_shapes=[
            pltpu.VMEM((chips, rows, width), bf16),
            pltpu.VMEM((chips, rows, width), bf16),
            pltpu.VMEM((tps - 1, chips, rows, cols), bf16),
            pltpu.VMEM((chips, rows, cols), bf16),
            pltpu.VMEM((chips, rows, cols), bf16),
            dma((chips,)), dma((chips,)), dma((chips,)),
            dma((tps - 1, chips)), dma((tps - 1, chips)), dma((chips,)), dma((chips,)),
        ],
        compiler_params=pltpu.CompilerParams(
            collective_id=1, has_side_effects=True, vmem_limit_bytes=min(60, 8 + 16 * chips * rows * width // 2**20 // 2) * 2**20
        ),
        cost_estimate=pl.CostEstimate(flops=200_000_000, bytes_accessed=20_000_000, transcendentals=0),
    )(partial.reshape(n, rows, width), shared_part)


def per_device(
    sizes,
    tokens,
    routes,
    route_weights,
    norm_gain,
    gate_experts,
    up_experts,
    down_experts,
    shared_gate,
    shared_up,
    shared_down,
):
    bf16, f32 = jnp.bfloat16, jnp.float32
    groups, n, tps = sizes
    width = tokens.shape[1] * tps
    experts_all = gate_experts.shape[0]
    held = experts_all // n
    gain_rows = norm_gain[None, :, None]
    chosen = routes[:, :, None] == jnp.arange(experts_all, dtype=jnp.int32)[None, None, :]
    per_expert = jnp.sum(jnp.where(chosen, route_weights[:, :, None], 0.0), axis=1)
    count = tokens.shape[0]
    scales = jnp.pad(per_expert.T, ((0, 0), (0, -count % 128)))
    weights = (
        (gate_experts * gain_rows).astype(bf16),
        (up_experts * gain_rows).astype(bf16),
        down_experts.astype(bf16),
        (shared_gate[None] * gain_rows).astype(bf16),
        (shared_up[None] * gain_rows).astype(bf16),
        shared_down[None].astype(bf16),
    )
    if fused_fits(sizes, tokens, scales, *weights):
        mixed, gate_local, up_local, down_local, sg, su, sd = fused(sizes, tokens, scales, *weights)
        return mixed, gate_local, up_local, down_local, sg[0], su[0], sd[0]
    moved = move(sizes, tokens, scales, *weights)
    everyone, scales, gate_local, up_local, down_local, sg, su, sd = moved
    sg, su, sd = sg[0], su[0], sd[0]
    here = lax.axis_index("fs")
    widened = everyone.reshape(n * count, width).astype(f32)
    rows = (widened * lax.rsqrt(jnp.mean(widened * widened, axis=1, keepdims=True) + 1e-06)).astype(bf16)
    normed = lax.dynamic_slice_in_dim(rows, here * count, count, 0)
    scale = lax.dynamic_slice_in_dim(scales, here * held, held, 1)[:, :, :count]
    scale = scale.transpose(0, 2, 1).reshape(n * count, held)

    def hidden(x, g, u):
        return jax.nn.silu(jnp.dot(x, g, preferred_element_type=f32)) * jnp.dot(x, u, preferred_element_type=f32)

    active = jnp.concatenate(
        [(hidden(rows, gate_local[j], up_local[j]) * scale[:, j:j + 1]).astype(bf16) for j in range(held)], axis=1
    )
    partial = jnp.dot(active, down_local.reshape(-1, width), preferred_element_type=f32).astype(bf16)
    shared_part = jnp.dot(hidden(normed, sg, su).astype(bf16), sd, preferred_element_type=f32)
    mixed = combine(sizes, partial, shared_part)
    return mixed, gate_local, up_local, down_local, sg, su, sd


def solution(mesh):
    sizes = (mesh.shape["grp"], mesh.shape["fs"], mesh.shape["tp"])
    return jax.shard_map(
        functools.partial(per_device, sizes),
        mesh=mesh,
        in_specs=(
            P(("grp", "fs"), "tp"),
            P(("grp", "fs"), None),
            P(("grp", "fs"), None),
            P("fs"),
            P(None, "fs", "tp"),
            P(None, "fs", "tp"),
            P(None, "fs", "tp"),
            P("fs", "tp"),
            P("fs", "tp"),
            P("fs", "tp"),
        ),
        out_specs=(
            P(("grp", "fs"), "tp"),
            P(("grp", "fs"), None, "tp"),
            P(("grp", "fs"), None, "tp"),
            P(("grp", "fs"), "tp", None),
            P("grp", "tp"),
            P("grp", "tp"),
            P(("grp", "tp"), None),
        ),
        check_vma=False,
    )
```
